512 devices in a mesh: ep: 32 (over z, core), tp: 16 (over y, x).
Axes of the slice: x: 4, y: 4, z: 16, core: 2. Of those that a mesh axis runs over, the one named last changes fastest.
Arguments:
- query_rows: bfloat16 [24576, 1024], P('ep', 'tp'), may hold values from -600 to 600
- key_rows: bfloat16 [24576, 1024], P('ep', 'tp'), may hold values from -6 to 6
- value_rows: bfloat16 [24576, 1024], P('ep', 'tp'), may hold values from -6 to 6
- cum_gate: float32 [16, 24576], P('tp'), may hold values from -2458 to 0, as said below
- out_weight: bfloat16 [1024, 2048], P(None, 'tp'), may hold values from -0.1875 to 0.1875
- moe_input: bfloat16 [6144, 2048], P('ep'), may hold values from -6 to 6
- moe_gain: float32 [2048], replicated, may hold values from 0.1 to 1.9
- routes: int32 [6144, 3], P('ep'), may hold values from 0 to 127, all different within a row; in each aligned block of 192 rows (0 to 191, 192 to 383, ...) at most 9 rows name the same one
- route_weight: float32 [6144, 3], P('ep'), may hold values from 0.2 to 1.5
- expert_gate: bfloat16 [128, 2048, 512], P('ep', None, 'tp'), may hold values from -0.125 to 0.125
- expert_up: bfloat16 [128, 2048, 512], P('ep', None, 'tp'), may hold values from -0.125 to 0.125
- expert_down: bfloat16 [128, 512, 2048], P('ep', None, 'tp'), may hold values from -0.25 to 0.25
- shared_gate: bfloat16 [2048, 512], P(None, 'tp'), may hold values from -0.125 to 0.125
- shared_up: bfloat16 [2048, 512], P(None, 'tp'), may hold values from -0.125 to 0.125
- shared_down: bfloat16 [512, 2048], P(None, 'tp'), may hold values from -0.25 to 0.25
Outputs:
- mixer_out: bfloat16 [24576, 2048], P('ep', 'tp')
- moe_out: bfloat16 [6144, 2048], P('ep', 'tp')
The draws below stay inside these ranges and needn't reach their ends.
Inputs may be any that keep to these rules, and one draw needn't show every extreme that they name: Non-increasing along positions: cum_gate[h, t] is the sum of the log forget gates of head h over positions 0 to t. `routes`: the 3 experts of a token differ. In each aligned block of 192 tokens no expert is named by more than 9 tokens, a bound that some block reaches.
All inputs are finite; a program needn't handle non-finite values.
Results may differ from the reference program's by a relative error of at most 0.0068.
Values may be sent and summed in bfloat16 or wider, within the bound.
No kernel may reach another device: no remote copies, remote signals or barrier semaphores. Data moves between devices by JAX's collectives and lax.ppermute only.
A program may use at most 64 MiB of HBM per device.

```python
import math
import jax
import jax.numpy as jnp
import numpy as np
from jax import lax

D = 2048
HEADS = 16
HEAD = 64
FF = 512
FS = 512
EXPERTS = 128
TOP = 3
SEQ_DEV = 768
LENGTH = 24576
MOE_DEV = 192
TOKENS_MOE = 6144
CAP = 9
N_EP = 32


def draw_query_rows(key, part):
    base_key = jax.random.fold_in(key, 7)
    key_normal = jax.random.fold_in(base_key, 0)
    drawn = jnp.clip(jax.random.normal(key_normal, (LENGTH, HEADS * HEAD), jnp.float32), -6.0, 6.0)
    return drawn.astype(jnp.bfloat16)


def draw_cum_gate(key, part):
    base_key = jax.random.fold_in(key, 13)
    key_heads, key_steps, key_blocks = jax.random.split(base_key, 3)
    head_order = jax.random.permutation(key_heads, HEADS)
    fast_count = HEADS // 2
    decay_rates = jnp.where(head_order < fast_count, 1.0 / 40.0, 1.0 / LENGTH).astype(jnp.float32)
    low = jnp.log(0.5)
    high = jnp.log(2.0)
    step_factors = jnp.exp(jax.random.uniform(key_steps, (HEADS, LENGTH), jnp.float32, low, high))
    block_factors = jnp.exp(jax.random.uniform(key_blocks, (HEADS, LENGTH // SEQ_DEV), jnp.float32, low, high))
    block_factors = jnp.repeat(block_factors, SEQ_DEV, axis=1)
    log_gates = -decay_rates[:, None] * step_factors * block_factors
    return jnp.cumsum(log_gates, axis=1).astype(jnp.float32)


def levels(rng, shape, cuts, least, high):
    def one(axis_at, shards_of):
        draws = jax.random.uniform(jax.random.fold_in(jax.random.fold_in(rng, 6), axis_at), (shards_of,), jnp.float32, least / len(cuts), high / len(cuts))
        return jnp.repeat(jnp.exp(draws), shape[axis_at] // shards_of).reshape((-1,) + (1,) * (len(shape) - axis_at - 1))

    loudness = one(*cuts[0])
    for cut in cuts[1:]:
        loudness = loudness * one(*cut)
    return loudness


def deal_out(rng, own, number, rows, amount, top, limit, slope):
    order = jax.random.permutation(rng, amount)
    heavy_load, common = load_shares(amount, rows * top, limit, slope, True), load_shares(amount, rows * top, limit, slope, False)
    places = jnp.arange(amount)

    def named(tallies, turn):
        used = int((tallies > 0).sum())
        fixed = max(1, used // 4)
        shifted = fixed + (places - fixed + turn * (used - fixed)) % max(1, amount - fixed)
        return jnp.zeros((amount,), jnp.int32).at[order[jnp.where(places < fixed, places, shifted)]].set(jnp.asarray(tallies, jnp.int32))

    tallies = jnp.where(number % 4 == 0, named(heavy_load, number // 4), named(common, number - number // 4 - 1))
    mixed = jax.random.permutation(jax.random.fold_in(own, 3), amount)
    donor, receiver = mixed[0:amount // 2 * 2:2], mixed[1:amount // 2 * 2:2]
    margin = jnp.minimum(tallies[donor] - 1, limit - tallies[receiver]) // 2
    margin = jnp.where((donor == order[0]) | (receiver == order[0]) | (tallies[receiver] == 0), 0, jnp.maximum(margin, 0))
    shifted = jax.random.randint(jax.random.fold_in(own, 4), (amount // 2,), 0, 1 << 20) % (margin + 1)
    tallies = tallies.at[donor].add(-shifted).at[receiver].add(shifted)
    members = jnp.searchsorted(jnp.cumsum(tallies), jnp.arange(rows * top), side="right").astype(jnp.int32)
    listing = members.reshape(top, rows).T
    listing = listing[jax.random.permutation(jax.random.fold_in(own, 1), rows)]
    turn = jax.random.randint(jax.random.fold_in(own, 2), (rows, 1), 0, top)
    return jnp.take_along_axis(listing, (jnp.arange(top)[None, :] + turn) % top, axis=1)


def load_shares(amount, total, reach, skew, full):
    portions = [(1 << 20) // math.isqrt(standing ** skew) + 1 for standing in range(1, amount + 1)]
    largest = reach if full else min(reach, max(-(-total // amount), total * portions[0] // sum(portions)))
    least = 1 if total - largest >= amount - 1 else 0
    holding, rest = [largest] + [least] * (amount - 1), total - largest - least * (amount - 1)
    while rest > 0:
        free = [i for i in range(1, amount) if holding[i] < largest] or [i for i in range(1, amount) if holding[i] < reach]
        pool, left = sum([portions[i] for i in free]), rest
        for i in free:
            more = min(reach - holding[i], max(1, left * portions[i] // pool), rest)
            holding[i] = holding[i] + more
            rest = rest - more
    return np.array(holding)


def bell_draw(stream_key, shape, deviation, limit, cuts=(), kind=jnp.bfloat16):
    array = jax.random.normal(stream_key, shape, jnp.float32) * deviation
    if len(cuts) > 0:
        array = levels(stream_key, shape, cuts, -0.22, 0.18) * array
    return jnp.clip(array, min=-limit, max=limit).astype(kind)


def setup_inputs(seed: int = 0) -> dict:
    keys = jax.random.split(jax.random.key(seed), 16)
    query_rows = draw_query_rows(jax.random.fold_in(keys[15], 71), 0)
    key_rows = bell_draw(keys[1], (LENGTH, HEADS * HEAD), 1.0, 6.0, ((0, 32), (1, 16)))
    value_rows = bell_draw(keys[2], (LENGTH, HEADS * HEAD), 1.0, 6.0, ((0, 32), (1, 16)))
    cum_gate = draw_cum_gate(jax.random.fold_in(keys[15], 71), 0)
    out_weight = bell_draw(keys[4], (HEADS * HEAD, D), (HEADS * HEAD) ** -0.5, 0.1875, ((1, 16),))
    moe_input = bell_draw(keys[5], (TOKENS_MOE, D), 1.0, 6.0, ((0, 32),))
    moe_gain = jnp.clip(1.0 + 0.18 * jax.random.normal(keys[6], (D,), jnp.float32), 0.1, 1.9)
    routes_keys = jax.random.split(jax.random.fold_in(keys[7], 1), TOKENS_MOE // MOE_DEV)
    routes_turns = jax.random.permutation(jax.random.fold_in(keys[7], 3), TOKENS_MOE // MOE_DEV)
    routes = jax.vmap(lambda own, number: deal_out(jax.random.fold_in(keys[7], 2), own, number, MOE_DEV, EXPERTS, TOP, CAP, 2))(routes_keys, routes_turns).reshape((TOKENS_MOE, TOP))
    route_weight = jnp.clip(jnp.exp(math.log(1.5) - 2.014903 * jax.random.uniform(keys[8], (TOKENS_MOE, TOP), jnp.float32) ** levels(keys[8], (TOKENS_MOE, TOP), ((0, 32),), -0.2, 0.2)), 0.2, 1.5)
    expert_gate = bell_draw(keys[9], (EXPERTS, D, FF), D ** -0.5, 0.125, ((0, 32), (2, 16)))
    expert_up = bell_draw(keys[10], (EXPERTS, D, FF), D ** -0.5, 0.125, ((0, 32), (2, 16)))
    expert_down = bell_draw(keys[11], (EXPERTS, FF, D), FF ** -0.5, 0.25, ((0, 32), (2, 16)))
    shared_gate = bell_draw(keys[12], (D, FS), D ** -0.5, 0.125, ((1, 16),))
    shared_up = bell_draw(keys[13], (D, FS), D ** -0.5, 0.125, ((1, 16),))
    shared_down = bell_draw(keys[14], (FS, D), FS ** -0.5, 0.25, ((1, 16),))
    return {"query_rows": query_rows, "key_rows": key_rows, "value_rows": value_rows, "cum_gate": cum_gate, "out_weight": out_weight, "moe_input": moe_input, "moe_gain": moe_gain, "routes": routes, "route_weight": route_weight, "expert_gate": expert_gate, "expert_up": expert_up, "expert_down": expert_down, "shared_gate": shared_gate, "shared_up": shared_up, "shared_down": shared_down}


neg_fill = -1e+30
norm_eps = 1e-06

def attention_heads(query_rows, key_rows, value_rows, cum_gate):
    query_span = 128 if LENGTH % 128 == 0 else LENGTH
    query_heads = query_rows.reshape(LENGTH, HEADS, HEAD)
    key_heads = key_rows.reshape(LENGTH, HEADS, HEAD).astype(jnp.float32)
    value_heads = value_rows.reshape(LENGTH, HEADS, HEAD).astype(jnp.float32)
    key_pos = jnp.arange(LENGTH, dtype=jnp.int32)
    scale = HEAD ** (-0.5)

    def one_block(block_index):
        start = (block_index * query_span).astype(jnp.int32)
        query_block = lax.dynamic_slice_in_dim(query_heads, start, query_span, 0).astype(jnp.float32)
        query_gate = lax.dynamic_slice_in_dim(cum_gate, start, query_span, 1)
        scores = jnp.einsum('qhd,khd->hqk', query_block, key_heads) * scale
        scores = scores + query_gate[:, :, None] - cum_gate[:, None, :]
        query_pos = start + jnp.arange(query_span, dtype=jnp.int32)
        causal = key_pos[None, :] <= query_pos[:, None]
        scores = jnp.where(causal[None], scores, neg_fill)
        row_max = lax.optimization_barrier(jnp.max(scores, axis=2, keepdims=True))
        expon = jnp.where(causal[None], jnp.exp(scores - row_max), 0.0)
        denom = lax.optimization_barrier(jnp.sum(expon, axis=2))
        probs = lax.optimization_barrier(expon.astype(jnp.bfloat16)).astype(jnp.float32)
        summed = jnp.einsum('hqk,khd->qhd', probs, value_heads)
        result = summed / jnp.transpose(denom)[:, :, None]
        return result.astype(jnp.bfloat16).reshape(query_span, HEADS * HEAD)
    blocks = lax.map(one_block, jnp.arange(LENGTH // query_span, dtype=jnp.int32))
    return blocks.reshape(LENGTH, HEADS * HEAD)

def experts_branch(moe_input, moe_gain, routes, route_weight, expert_gate, expert_up, expert_down, shared_gate, shared_up, shared_down):
    moe_rows = moe_input.astype(jnp.float32)
    normed = (moe_rows * lax.rsqrt(lax.optimization_barrier(jnp.mean(moe_rows * moe_rows, axis=1, keepdims=True)) + norm_eps) * moe_gain).astype(jnp.bfloat16)
    pair_count = TOKENS_MOE * TOP
    flat_routes = routes.reshape(-1).astype(jnp.int32)
    one_hot = (flat_routes[:, None] == jnp.arange(EXPERTS, dtype=jnp.int32)[None, :]).astype(jnp.int32)
    one_hot = one_hot.reshape(N_EP, MOE_DEV * TOP, EXPERTS)
    ranks = lax.optimization_barrier(jnp.sum(jnp.cumsum(one_hot, axis=1) * one_hot, axis=2)).reshape(-1) - 1
    block_id = jnp.arange(pair_count, dtype=jnp.int32) // (MOE_DEV * TOP)
    slot_index = (flat_routes * (N_EP * CAP) + block_id * CAP + ranks).astype(jnp.int32)
    pair_token = jnp.arange(pair_count, dtype=jnp.int32) // TOP
    slot_token = jnp.full((EXPERTS * N_EP * CAP,), TOKENS_MOE, jnp.int32).at[slot_index].set(pair_token)
    padded = jnp.concatenate([normed, jnp.zeros((1, D), jnp.bfloat16)], axis=0)

    def one_expert(pieces):
        token_index, gate_w, up_w, down_w = pieces
        gathered = padded[token_index]
        gate_val = jnp.dot(gathered, gate_w, preferred_element_type=jnp.float32)
        up_val = jnp.dot(gathered, up_w, preferred_element_type=jnp.float32)
        hidden = (jax.nn.silu(gate_val) * up_val).astype(jnp.bfloat16)
        return jnp.dot(hidden, down_w, preferred_element_type=jnp.float32).astype(jnp.bfloat16)
    results = lax.map(one_expert, (slot_token.reshape(EXPERTS, N_EP * CAP), expert_gate, expert_up, expert_down))
    picked = results.reshape(EXPERTS * N_EP * CAP, D)[slot_index].astype(jnp.float32).reshape(TOKENS_MOE, TOP, D)
    routed = lax.optimization_barrier(jnp.sum(picked * route_weight[:, :, None], axis=1))
    shared_hidden = (jax.nn.silu(jnp.dot(normed, shared_gate, preferred_element_type=jnp.float32)) * jnp.dot(normed, shared_up, preferred_element_type=jnp.float32)).astype(jnp.bfloat16)
    total = routed + jnp.dot(shared_hidden, shared_down, preferred_element_type=jnp.float32)
    return total.astype(jnp.bfloat16)

def reference(query_rows, key_rows, value_rows, cum_gate, out_weight, moe_input, moe_gain, routes, route_weight, expert_gate, expert_up, expert_down, shared_gate, shared_up, shared_down):
    heads_out = attention_heads(query_rows, key_rows, value_rows, cum_gate)
    mixer_out = jnp.dot(heads_out, out_weight, preferred_element_type=jnp.float32).astype(jnp.bfloat16)
    moe_out = experts_branch(moe_input, moe_gain, routes, route_weight, expert_gate, expert_up, expert_down, shared_gate, shared_up, shared_down)
    return (mixer_out, moe_out)
```

```python
import functools

import jax
import jax.numpy as jnp
from jax import lax
from jax.experimental import pallas as pl
from jax.experimental.pallas import tpu as pltpu
from jax.sharding import PartitionSpec as P

HEAD = 64
CAP = 9
LOG2E = 1.4426950408889634
neg_fill = -1e30
norm_eps = 1e-06
F32 = jnp.float32
BF16 = jnp.bfloat16
NT = (((1,), (1,)), ((), ()))
TN = (((0,), (0,)), ((), ()))
NN = (((1,), (0,)), ((), ()))


def dot(a, b, dims=NN):
    return lax.dot_general(a, b, dims, preferred_element_type=F32)


def sent_to_all(array, axis):
    copies = jnp.broadcast_to(array, (lax.axis_size(axis), *array.shape))
    return lax.all_to_all(copies, axis, split_axis=0, concat_axis=0, tiled=True)


def cost(flops, nbytes):
    return pl.CostEstimate(flops=flops, transcendentals=0, bytes_accessed=nbytes)


def attention_kernel(ep_ref, q_ref, kv_ref, gk_ref, g0_ref, out_ref, q_scr, m_scr, acc_scr, *, tile):
    step = pl.program_id(0)
    own = ep_ref[0]
    rows = q_scr.shape[0]
    keys = kv_ref.shape[2]

    @pl.when(step == 0)
    def _():
        q_scr[...] = q_ref[...].T
        m_scr[...] = jnp.full(m_scr.shape, neg_fill, F32)
        acc_scr[...] = jnp.zeros(acc_scr.shape, F32)

    def update(diagonal):
        kt = kv_ref[0, :HEAD, :]
        row_id = lax.broadcasted_iota(jnp.int32, (2 * HEAD, keys), 0)
        vt = jnp.where(row_id < HEAD, jnp.ones((), BF16), kv_ref[0].astype(BF16))
        gate = (gk_ref[...] - g0_ref[:, :1]) * LOG2E
        for i in range(rows // tile):
            span = pl.ds(i * tile, tile)
            used = min(keys, (i + 1) * tile) if diagonal else keys
            s = dot(q_scr[span, :], kt[:, :used]) * (LOG2E * HEAD**-0.5) - gate[:, :used]
            if diagonal:
                q_pos = i * tile + lax.broadcasted_iota(jnp.int32, (tile, used), 0)
                k_pos = lax.broadcasted_iota(jnp.int32, (tile, used), 1)
                s = jnp.where(k_pos <= q_pos, s, neg_fill)
            old = m_scr[span, :1]
            new = jnp.maximum(old, jnp.max(s, axis=1, keepdims=True))
            p = jnp.exp2(s - new).astype(BF16)
            acc_scr[span, :] = acc_scr[span, :] * jnp.exp2(old - new) + dot(p, vt[:, :used], NT)
            m_scr[span, :] = jnp.broadcast_to(new, (tile, m_scr.shape[1]))

    @pl.when(step == 0)
    def _():
        update(True)

    @pl.when((step > 0) & (step <= own))
    def _():
        update(False)

    @pl.when(step == pl.num_programs(0) - 1)
    def _():
        half = rows // 2
        top = acc_scr[:half, :]
        low = acc_scr[half:, :]
        out_ref[...] = jnp.concatenate(
            [top[:, HEAD:] / top[:, :HEAD], low[:, HEAD:] / low[:, :HEAD]], axis=1
        ).astype(BF16)


def attention(ep_index, q_t, kv_all, cum_gate):
    blocks, wide, keys = kv_all.shape
    rows = q_t.shape[1]

    def place(j, ep):
        return jnp.where(j == 0, ep[0], jnp.maximum(jnp.minimum(j, ep[0]) - 1, 0))

    return pl.pallas_call(
        functools.partial(attention_kernel, tile=256),
        grid_spec=pltpu.PrefetchScalarGridSpec(
            num_scalar_prefetch=1,
            grid=(blocks,),
            in_specs=[
                pl.BlockSpec((HEAD, rows), lambda j, ep: (0, 0)),
                pl.BlockSpec((1, wide, keys), lambda j, ep: (place(j, ep), 0, 0)),
                pl.BlockSpec((1, keys), lambda j, ep: (0, place(j, ep))),
                pl.BlockSpec((1, keys), lambda j, ep: (0, ep[0])),
            ],
            out_specs=pl.BlockSpec((rows // 2, 2 * HEAD), lambda j, ep: (0, 0)),
            scratch_shapes=[
                pltpu.VMEM((rows, HEAD), BF16),
                pltpu.VMEM((rows, 128), F32),
                pltpu.VMEM((rows, 128), F32),
            ],
        ),
        out_shape=jax.ShapeDtypeStruct((rows // 2, 2 * HEAD), BF16),
        compiler_params=pltpu.CompilerParams(dimension_semantics=("arbitrary",)),
        cost_estimate=cost(2 * 2 * rows * keys * blocks * 256, 8 << 20),
        name="attention",
    )(ep_index, q_t, kv_all, cum_gate, cum_gate)


def projection_kernel(heads_ref, w_ref, out_ref):
    count, half, _ = heads_ref.shape
    acc = jnp.zeros((half, 2 * w_ref.shape[1]), F32)
    blank = jnp.zeros((HEAD, w_ref.shape[1]), BF16)
    for h in range(count):
        w = w_ref[h * HEAD : (h + 1) * HEAD, :]
        both = jnp.concatenate(
            [jnp.concatenate([w, blank], axis=1), jnp.concatenate([blank, w], axis=1)], axis=0
        )
        acc = acc + dot(heads_ref[h], both)
    out_ref[:half, :] = acc[:, : w_ref.shape[1]].astype(BF16)
    out_ref[half:, :] = acc[:, w_ref.shape[1] :].astype(BF16)


def projection(heads, out_weight):
    count, half, _ = heads.shape
    columns = out_weight.shape[1]
    return pl.pallas_call(
        projection_kernel,
        out_shape=jax.ShapeDtypeStruct((2 * half, columns), BF16),
        cost_estimate=cost(2 * half * count * 128 * 256, 4 << 20),
        name="projection",
    )(heads, out_weight)


def spread_kernel(gate_ref, up_ref, out_ref):
    peers = out_ref.shape[0]
    for t in range(peers):
        out_ref[t, 0] = gate_ref[:, :, t * 128 : (t + 1) * 128]
        out_ref[t, 1] = up_ref[:, :, t * 128 : (t + 1) * 128]


def spread_weights(gate_t, up_t, peers):
    experts, hidden, width = gate_t.shape
    return pl.pallas_call(
        spread_kernel,
        out_shape=jax.ShapeDtypeStruct((peers, 2, experts, hidden, width // peers), BF16),
        name="spread",
    )(gate_t, up_t)


def route_kernel(
    tp_ref, x_ref, gain_ref, routes_ref, weight_ref, sg_ref, su_ref, slot_ref, mix_ref, shared_ref, norm_scr,
    *, groups, local_experts, room,
):
    tokens = x_ref.shape[0]
    x = x_ref[...].astype(F32)
    scale = lax.rsqrt(jnp.mean(x * x, axis=1, keepdims=True) + norm_eps)
    normed = (x * scale * gain_ref[...]).astype(BF16)
    norm_scr[...] = normed
    columns = slot_ref.shape[1]
    piece = norm_scr[:, pl.ds(pl.multiple_of(tp_ref[0] * columns, columns), columns)]
    slots = groups * room
    shape = (groups, room, tokens)
    within = lax.broadcasted_iota(jnp.int32, shape, 1)
    expert = lax.broadcasted_iota(jnp.int32, shape, 0) * local_experts + within % local_experts
    expert = expert.reshape(slots, tokens)
    turn = (within // local_experts).reshape(slots, tokens).astype(F32)
    hit = jnp.zeros((slots, tokens), F32)
    weight = jnp.zeros((slots, tokens), F32)
    for j in range(routes_ref.shape[0]):
        same = expert == routes_ref[j : j + 1, :]
        hit = hit + jnp.where(same, 1.0, 0.0)
        weight = weight + jnp.where(same, weight_ref[j : j + 1, :], 0.0)
    before = lax.broadcasted_iota(jnp.int32, (tokens, tokens), 0)
    after = lax.broadcasted_iota(jnp.int32, (tokens, tokens), 1)
    earlier = jnp.where(before < after, 1.0, 0.0).astype(BF16)
    rank = dot(hit.astype(BF16), earlier)
    chosen = jnp.where(rank == turn, hit, 0.0)
    slot_ref[...] = dot(chosen.astype(BF16), piece).astype(BF16)
    mix = chosen * weight
    coarse = mix.astype(BF16)
    mix_ref[0] = coarse
    mix_ref[1] = (mix - coarse.astype(F32)).astype(BF16)
    gate_val = dot(sg_ref[...], normed, NT)
    up_val = dot(su_ref[...], normed, NT)
    shared_ref[...] = (gate_val / (1.0 + jnp.exp(-gate_val)) * up_val).astype(BF16)


def route(tp_index, x, gain, routes_t, weight_t, sg_t, su_t, groups, local_experts, room, columns):
    tokens, width = x.shape
    slots = groups * room
    whole = pl.BlockSpec(memory_space=pltpu.VMEM)
    return pl.pallas_call(
        functools.partial(route_kernel, groups=groups, local_experts=local_experts, room=room),
        in_specs=[pl.BlockSpec(memory_space=pltpu.SMEM)] + [whole] * 6,
        out_specs=(whole, whole, whole),
        out_shape=(
            jax.ShapeDtypeStruct((slots, columns), BF16),
            jax.ShapeDtypeStruct((2, slots, tokens), BF16),
            jax.ShapeDtypeStruct((sg_t.shape[0], tokens), BF16),
        ),
        scratch_shapes=[pltpu.VMEM((tokens, width), BF16)],
        name="route",
    )(tp_index, x, gain, routes_t, weight_t, sg_t, su_t)


def by_expert(rows, count):
    own = lax.broadcasted_iota(jnp.int32, rows.shape, 0) % count
    return jnp.concatenate([jnp.where(own == e, rows, jnp.zeros((), rows.dtype)) for e in range(count)], axis=1)


def partial_kernel(rows_ref, w_ref, out_ref):
    peers, _, count, hidden, depth = w_ref.shape
    spread = by_expert(rows_ref[...], count)
    for g in range(2):
        w = jnp.concatenate([w_ref[:, g, e].reshape(peers * hidden, depth) for e in range(count)], axis=1)
        out_ref[:, g * peers * hidden : (g + 1) * peers * hidden] = dot(spread, w, NT).astype(BF16)


def partial_products(rows, weights):
    peers, _, count, hidden, _ = weights.shape
    return pl.pallas_call(
        partial_kernel,
        out_shape=jax.ShapeDtypeStruct((rows.shape[0], 2 * peers * hidden), BF16),
        name="partial",
    )(rows, weights)


def activate_kernel(parts_ref, out_ref):
    total = parts_ref[0].astype(F32)
    for t in range(1, parts_ref.shape[0]):
        total = total + parts_ref[t].astype(F32)
    half = out_ref.shape[1]
    gate_val = total[:, :half]
    out_ref[...] = (gate_val / (1.0 + jnp.exp(-gate_val)) * total[:, half:]).astype(BF16)


def activate(parts):
    _, rows, width = parts.shape
    return pl.pallas_call(
        activate_kernel,
        out_shape=jax.ShapeDtypeStruct((rows, width // 2), BF16),
        name="activate",
    )(parts)


def down_kernel(rows_ref, w_ref, out_ref):
    count, hidden, columns = w_ref.shape
    spread = by_expert(rows_ref[...], count)
    out_ref[...] = dot(spread, w_ref[...].reshape(count * hidden, columns)).astype(BF16)


def down(rows, weights):
    return pl.pallas_call(
        down_kernel,
        out_shape=jax.ShapeDtypeStruct((rows.shape[0], weights.shape[2]), BF16),
        name="down",
    )(rows, weights)


def combine_kernel(mix_ref, back_ref, shared_ref, w_ref, out_ref):
    back = back_ref[...]
    routed = dot(mix_ref[0], back, TN) + dot(mix_ref[1], back, TN)
    out_ref[...] = (routed + dot(shared_ref[...], w_ref[...], TN)).astype(BF16)


def combine(mix, back, shared, shared_down):
    return pl.pallas_call(
        combine_kernel,
        out_shape=jax.ShapeDtypeStruct((mix.shape[2], back.shape[1]), BF16),
        name="combine",
    )(mix, back, shared, shared_down)


def local(
    query_rows,
    key_rows,
    value_rows,
    cum_gate,
    out_weight,
    moe_input,
    moe_gain,
    routes,
    route_weight,
    expert_gate,
    expert_up,
    expert_down,
    shared_gate,
    shared_up,
    shared_down,
):
    groups = lax.axis_size("ep")
    peers = lax.axis_size("tp")
    ep_index = lax.axis_index("ep").astype(jnp.int32).reshape(1)
    tp_index = lax.axis_index("tp").astype(jnp.int32).reshape(1)
    local_experts = expert_gate.shape[0]
    columns = expert_down.shape[2]
    room = -(-CAP * local_experts // 8) * 8
    key_value = jnp.concatenate([key_rows.T, value_rows.T], axis=0)
    kv_all = lax.all_gather(key_value, "ep", axis=0)
    weights = lax.all_to_all(
        spread_weights(expert_gate.transpose(0, 2, 1), expert_up.transpose(0, 2, 1), peers).reshape(
            peers, -1, 128
        ),
        "tp", split_axis=0, concat_axis=0, tiled=True,
    )
    slots, mix, shared = route(
        tp_index, moe_input, moe_gain.reshape(1, -1), routes.T, route_weight.T, shared_gate.T, shared_up.T,
        groups, local_experts, room, columns,
    )
    arrived = lax.all_to_all(slots.reshape(groups, room, columns), "ep", split_axis=0, concat_axis=0, tiled=True)
    shared_all = sent_to_all(shared, "tp")
    parts = partial_products(
        arrived.reshape(groups * room, columns),
        weights.reshape(peers, 2, local_experts, expert_gate.shape[2], 128),
    )
    parts = lax.all_to_all(
        parts.reshape(peers, groups * room // peers, -1), "tp", split_axis=0, concat_axis=0, tiled=True
    )
    hidden = sent_to_all(activate(parts), "tp")
    result = down(hidden.reshape(groups * room, -1), expert_down)
    back = lax.all_to_all(result.reshape(groups, room, columns), "ep", split_axis=0, concat_axis=0, tiled=True)
    heads = attention(ep_index, query_rows.T, kv_all, cum_gate)
    mixer_out = projection(sent_to_all(heads, "tp"), out_weight)
    moe_out = combine(mix, back.reshape(groups * room, columns), shared_all.reshape(-1, shared_all.shape[2]), shared_down)
    return (mixer_out, moe_out)


def solution(mesh):
    placed = (
        P("ep", "tp"),
        P("ep", "tp"),
        P("ep", "tp"),
        P("tp", None),
        P(None, "tp"),
        P("ep", None),
        P(),
        P("ep", None),
        P("ep", None),
        P("ep", None, "tp"),
        P("ep", None, "tp"),
        P("ep", None, "tp"),
        P(None, "tp"),
        P(None, "tp"),
        P(None, "tp"),
    )
    return jax.shard_map(
        local, mesh=mesh, in_specs=placed, out_specs=(P("ep", "tp"), P("ep", "tp")), check_vma=False
    )
```

```python
import functools
import math

import jax
import jax.numpy as jnp
from jax import lax
from jax.experimental import pallas as pl
from jax.experimental.pallas import tpu as pltpu
from jax.sharding import PartitionSpec as P

HEAD = 64
CAP = 9
LOG2E = 1.4426950408889634
neg_fill = -1e30
norm_eps = 1e-06
F32 = jnp.float32
BF16 = jnp.bfloat16
NT = (((1,), (1,)), ((), ()))
TN = (((0,), (0,)), ((), ()))
NN = (((1,), (0,)), ((), ()))


def dot(a, b, dims=NN):
    return lax.dot_general(a, b, dims, preferred_element_type=F32)


def exchanged(array, axis, among=None):
    return lax.all_to_all(array, axis, split_axis=0, concat_axis=0, tiled=True, axis_index_groups=among)


def sent_to_all(array, axis, among=None):
    count = len(among[0]) if among else lax.axis_size(axis)
    return exchanged(jnp.broadcast_to(array, (count, *array.shape)), axis, among)


def cost(flops, nbytes):
    return pl.CostEstimate(flops=flops, transcendentals=0, bytes_accessed=nbytes)


HEADROOM = 64.0
EXTRA = 16


def three(x):
    first = x.astype(BF16)
    rest = x - first.astype(F32)
    second = rest.astype(BF16)
    return first, second, (rest - second.astype(F32)).astype(BF16)


def attention_kernel(ep_ref, *refs, tile, opening):
    if opening:
        q_ref, kv_ref, gk_ref, g0_ref, _, acc_out, m_out, q_scr, m_scr, acc_scr = refs
    else:
        q_ref, kv_ref, gk_ref, g0_ref, acc_in, m_in, _, out_ref, q_scr, m_scr, acc_scr = refs
    step = pl.program_id(0)
    own = ep_ref[0]
    count = own // 2 if opening else own - own // 2
    rows = q_scr.shape[0]
    keys = kv_ref.shape[2]

    def operands():
        kt = kv_ref[0, :HEAD, :]
        row_id = lax.broadcasted_iota(jnp.int32, (2 * HEAD, keys), 0)
        vt = jnp.where(row_id < HEAD, jnp.ones((), BF16), kv_ref[0])
        gate = (gk_ref[...] - g0_ref[:, :1]) * LOG2E
        row_id = lax.broadcasted_iota(jnp.int32, (EXTRA, keys), 0)
        gates = jnp.zeros((EXTRA, keys), F32)
        for n, piece in enumerate(three(gate)):
            gates = jnp.where(row_id == n, piece.astype(F32), gates)
        return jnp.concatenate([kt, kt, kt, gates.astype(BF16)], axis=0), vt

    def exact(source, target, diagonal):
        kx, vt = operands()
        for i in range(rows // tile):
            span = pl.ds(i * tile, tile)
            used = min(keys, (i + 1) * tile) if diagonal else keys
            s = dot(q_scr[span, :], kx[:, :used])
            if diagonal:
                q_pos = i * tile + lax.broadcasted_iota(jnp.int32, (tile, used), 0)
                k_pos = lax.broadcasted_iota(jnp.int32, (tile, used), 1)
                s = jnp.where(k_pos <= q_pos, s, neg_fill)
            top = jnp.max(s, axis=1, keepdims=True)
            if diagonal:
                p = jnp.exp2(s - top).astype(BF16)
                acc_scr[target, span, :] = dot(p, vt[:, :used], NT)
                m_scr[span, :] = jnp.broadcast_to(top, (tile, m_scr.shape[1]))
            else:
                old = m_scr[span, :]
                new = jnp.maximum(old, top)
                p = jnp.exp2(s - new[:, :1]).astype(BF16)
                acc_scr[target, span, :] = acc_scr[source, span, :] * jnp.exp2(old - new) + dot(p, vt, NT)
                m_scr[span, :] = new

    @pl.when(step == 0)
    def _():
        for n, piece in enumerate(three(q_ref[...].T.astype(F32) * (LOG2E * HEAD**-0.5))):
            q_scr[:, n * HEAD : (n + 1) * HEAD] = piece
        q_scr[:, 3 * HEAD :] = jnp.full((rows, EXTRA), -1.0, BF16)
        if opening:
            exact(0, 0, True)
        else:
            acc_scr[0] = acc_in[...]
            m_scr[...] = m_in[...]

    @pl.when((step > 0) & (step <= count))
    def _():
        source = (step - 1) % 2
        target = step % 2
        kx, vt = operands()
        worst = jnp.full((8, 128), neg_fill, F32)
        for i in range(rows // tile):
            span = pl.ds(i * tile, tile)
            x = dot(q_scr[span, :], kx) - m_scr[span, :1]
            most = x[:, :128]
            for c in range(128, keys, 128):
                most = jnp.maximum(most, x[:, c : c + 128])
            worst = jnp.maximum(worst, jnp.max(most.reshape(tile // 8, 8, 128), axis=0))
            acc_scr[target, span, :] = acc_scr[source, span, :] + dot(jnp.exp2(x).astype(BF16), vt, NT)

        @pl.when(jnp.max(worst) > HEADROOM)
        def _():
            exact(source, target, False)

    @pl.when(step == pl.num_programs(0) - 1)
    def _():
        last = count % 2
        if opening:
            acc_out[...] = acc_scr[last]
            m_out[...] = m_scr[...]
        else:
            half = rows // 2
            top = acc_scr[last, :half, :]
            low = acc_scr[last, half:, :]
            out_ref[...] = jnp.concatenate(
                [top[:, HEAD:] / top[:, :HEAD], low[:, HEAD:] / low[:, :HEAD]], axis=1
            ).astype(BF16)


def attention(ep_index, q_t, kv_all, cum_gate, state, after):
    blocks, wide, keys = kv_all.shape
    rows = q_t.shape[1]
    opening = state is None

    def place(j, ep):
        own = ep[0]
        half = own // 2
        if opening:
            return jnp.where(j == 0, own, jnp.maximum(jnp.minimum(j, half) - 1, 0))
        return jnp.minimum(half + jnp.maximum(j - 1, 0), jnp.maximum(own - 1, 0))

    flat = pl.BlockSpec((rows, 128), lambda j, ep: (0, 0))
    wide_f32 = jax.ShapeDtypeStruct((rows, 128), F32)
    return pl.pallas_call(
        functools.partial(attention_kernel, tile=384, opening=opening),
        grid_spec=pltpu.PrefetchScalarGridSpec(
            num_scalar_prefetch=1,
            grid=(blocks // 2 + (0 if opening else 1),),
            in_specs=[
                pl.BlockSpec((HEAD, rows), lambda j, ep: (0, 0)),
                pl.BlockSpec((1, wide, keys), lambda j, ep: (place(j, ep), 0, 0)),
                pl.BlockSpec((1, keys), lambda j, ep: (0, place(j, ep))),
                pl.BlockSpec((1, keys), lambda j, ep: (0, ep[0])),
            ]
            + ([] if opening else [flat, flat])
            + [pl.BlockSpec(memory_space=pl.ANY)],
            out_specs=(flat, flat) if opening else pl.BlockSpec((rows // 2, 2 * HEAD), lambda j, ep: (0, 0)),
            scratch_shapes=[
                pltpu.VMEM((rows, 3 * HEAD + EXTRA), BF16),
                pltpu.VMEM((rows, 128), F32),
                pltpu.VMEM((2, rows, 128), F32),
            ],
        ),
        out_shape=(wide_f32, wide_f32) if opening else jax.ShapeDtypeStruct((rows // 2, 2 * HEAD), BF16),
        compiler_params=pltpu.CompilerParams(dimension_semantics=("arbitrary",)),
        cost_estimate=cost(2 * rows * keys * blocks * 256, 4 << 20),
        name="attention_first" if opening else "attention_rest",
    )(ep_index, q_t, kv_all, cum_gate, cum_gate, *(state or ()), after)


def projection_kernel(heads_ref, w_ref, out_ref):
    count, half, _ = heads_ref.shape
    acc = jnp.zeros((half, 2 * w_ref.shape[1]), F32)
    blank = jnp.zeros((HEAD, w_ref.shape[1]), BF16)
    for h in range(count):
        w = w_ref[h * HEAD : (h + 1) * HEAD, :]
        both = jnp.concatenate(
            [jnp.concatenate([w, blank], axis=1), jnp.concatenate([blank, w], axis=1)], axis=0
        )
        acc = acc + dot(heads_ref[h], both)
    out_ref[:half, :] = acc[:, : w_ref.shape[1]].astype(BF16)
    out_ref[half:, :] = acc[:, w_ref.shape[1] :].astype(BF16)


def projection(heads, out_weight):
    count, half, _ = heads.shape
    columns = out_weight.shape[1]
    return pl.pallas_call(
        projection_kernel,
        out_shape=jax.ShapeDtypeStruct((2 * half, columns), BF16),
        cost_estimate=cost(2 * half * count * 128 * 256, 4 << 20),
        name="projection",
    )(heads, out_weight)


def spread_kernel(side_ref, gate_ref, up_ref, sg_ref, su_ref, *out_refs):
    side = len(out_refs)
    experts, hidden, width = gate_ref.shape
    part = width // side
    block = experts * hidden
    for k, out_ref in enumerate(out_refs):
        lanes = pl.ds(pl.multiple_of(lax.rem(side_ref[1] + k, side) * part, part), part)
        out_ref[:block, :] = gate_ref[:, :, lanes].reshape(block, part)
        out_ref[block : 2 * block, :] = up_ref[:, :, lanes].reshape(block, part)
        out_ref[2 * block : 2 * block + hidden, :] = sg_ref[:, lanes]
        out_ref[2 * block + hidden :, :] = su_ref[:, lanes]


def spread_weights(side_index, gate_t, up_t, sg_t, su_t, side):
    experts, hidden, width = gate_t.shape
    whole = pl.BlockSpec(memory_space=pltpu.VMEM)
    rows = 2 * (experts + 1) * hidden
    return pl.pallas_call(
        spread_kernel,
        in_specs=[pl.BlockSpec(memory_space=pltpu.SMEM)] + [whole] * 4,
        out_specs=[whole] * side,
        out_shape=[jax.ShapeDtypeStruct((rows, width // side), BF16)] * side,
        name="spread",
    )(side_index, gate_t, up_t, sg_t, su_t)


def route_kernel(
    side_ref, x_ref, gain_ref, routes_ref, weight_ref, slot_ref, mix_ref, part_ref, norm_scr,
    *, side, groups, local_experts, room,
):
    tokens = x_ref.shape[0]
    x = x_ref[...].astype(F32)
    scale = lax.rsqrt(jnp.mean(x * x, axis=1, keepdims=True) + norm_eps)
    norm_scr[...] = (x * scale * gain_ref[...]).astype(BF16)
    columns = slot_ref.shape[1]
    wide = part_ref.shape[1]
    part_ref[...] = norm_scr[:, pl.ds(pl.multiple_of(side_ref[1] * wide, wide), wide)]
    start = pl.multiple_of((side_ref[1] * side + side_ref[0]) * columns, columns)
    piece = norm_scr[:, pl.ds(start, columns)]
    slots = groups * room
    shape = (groups, room, tokens)
    within = lax.broadcasted_iota(jnp.int32, shape, 1)
    expert = lax.broadcasted_iota(jnp.int32, shape, 0) * local_experts + within % local_experts
    expert = expert.reshape(slots, tokens)
    turn = (within // local_experts).reshape(slots, tokens).astype(F32)
    hit = jnp.zeros((slots, tokens), F32)
    weight = jnp.zeros((slots, tokens), F32)
    for j in range(routes_ref.shape[0]):
        same = expert == routes_ref[j : j + 1, :]
        hit = hit + jnp.where(same, 1.0, 0.0)
        weight = weight + jnp.where(same, weight_ref[j : j + 1, :], 0.0)
    before = lax.broadcasted_iota(jnp.int32, (tokens, tokens), 0)
    after = lax.broadcasted_iota(jnp.int32, (tokens, tokens), 1)
    earlier = jnp.where(before < after, 1.0, 0.0).astype(BF16)
    rank = dot(hit.astype(BF16), earlier)
    chosen = jnp.where(rank == turn, hit, 0.0)
    slot_ref[...] = dot(chosen.astype(BF16), piece).astype(BF16)
    mix = chosen * weight
    coarse = mix.astype(BF16)
    mix_ref[0] = coarse
    mix_ref[1] = (mix - coarse.astype(F32)).astype(BF16)


def route(side_index, x, gain, routes_t, weight_t, side, groups, local_experts, room, columns):
    tokens, width = x.shape
    slots = groups * room
    whole = pl.BlockSpec(memory_space=pltpu.VMEM)
    return pl.pallas_call(
        functools.partial(route_kernel, side=side, groups=groups, local_experts=local_experts, room=room),
        in_specs=[pl.BlockSpec(memory_space=pltpu.SMEM)] + [whole] * 4,
        out_specs=(whole, whole, whole),
        out_shape=(
            jax.ShapeDtypeStruct((slots, columns), BF16),
            jax.ShapeDtypeStruct((2, slots, tokens), BF16),
            jax.ShapeDtypeStruct((tokens, width // side), BF16),
        ),
        scratch_shapes=[pltpu.VMEM((tokens, width), BF16)],
        name="route",
    )(side_index, x, gain, routes_t, weight_t)


def by_expert(rows, count):
    own = lax.broadcasted_iota(jnp.int32, rows.shape, 0) % count
    return jnp.concatenate([jnp.where(own == e, rows, jnp.zeros((), rows.dtype)) for e in range(count)], axis=1)


def partial_kernel(side_ref, rows_ref, tokens_ref, *refs, count, hidden):
    side = len(refs) - 3
    out_ref, w_scr, shared_scr = refs[side:]
    wide = side * hidden
    depth = rows_ref.shape[2]
    for k in range(side):
        place = pl.multiple_of(lax.rem(side_ref[1] + side - k, side) * hidden, hidden)
        for g in range(2):
            span = pl.ds(g * wide + place, hidden)
            for e in range(count):
                first = (g * count + e) * hidden
                for c in range(side):
                    lanes = (c * count + e) * depth
                    w_scr[span, lanes : lanes + depth] = refs[k][first : first + hidden, c * depth : (c + 1) * depth]
            first = (2 * count + g) * hidden
            shared_scr[span, :] = refs[k][first : first + hidden, :]
    each = rows_ref.shape[1] // side
    few = tokens_ref.shape[0] // side
    for n in range(side):
        total = jnp.zeros((each, 2 * wide), F32)
        for c in range(side):
            spread = by_expert(rows_ref[c, n * each : (n + 1) * each, :], count)
            total = total + dot(spread, w_scr[:, c * count * depth : (c + 1) * count * depth], NT)
        out_ref[n, :each, :] = total.astype(BF16)
        out_ref[n, each:, :] = dot(tokens_ref[n * few : (n + 1) * few, :], shared_scr[...], NT).astype(BF16)


def partial_products(side_index, rows, tokens, weights, count, hidden):
    side = len(weights)
    whole = pl.BlockSpec(memory_space=pltpu.VMEM)
    each = (rows.shape[1] + tokens.shape[0]) // side
    return pl.pallas_call(
        functools.partial(partial_kernel, count=count, hidden=hidden),
        in_specs=[pl.BlockSpec(memory_space=pltpu.SMEM)] + [whole] * (2 + side),
        out_specs=whole,
        out_shape=jax.ShapeDtypeStruct((side, each, 2 * side * hidden), BF16),
        scratch_shapes=[
            pltpu.VMEM((2 * side * hidden, count * side * rows.shape[2]), BF16),
            pltpu.VMEM((2 * side * hidden, tokens.shape[1]), BF16),
        ],
        name="partial",
    )(side_index, rows, tokens, *weights)


def activate_kernel(parts_ref, out_ref):
    total = parts_ref[0].astype(F32)
    for t in range(1, parts_ref.shape[0]):
        total = total + parts_ref[t].astype(F32)
    half = out_ref.shape[1]
    gate_val = total[:, :half]
    out_ref[...] = (gate_val / (1.0 + jnp.exp(-gate_val)) * total[:, half:]).astype(BF16)


def activate(parts):
    _, rows, width = parts.shape
    return pl.pallas_call(
        activate_kernel,
        out_shape=jax.ShapeDtypeStruct((rows, width // 2), BF16),
        name="activate",
    )(parts)


def down_kernel(hidden_ref, w_ref, sw_ref, out_ref, shared_ref, *, side):
    count, hidden, columns = w_ref.shape
    each = out_ref.shape[0] // side
    few = shared_ref.shape[0] // side
    w = w_ref[...].reshape(count * hidden, columns)
    for n in range(side):
        rows = jnp.concatenate([hidden_ref[y * side + n] for y in range(side)], axis=1)
        out_ref[n * each : (n + 1) * each, :] = dot(by_expert(rows[:each], count), w).astype(BF16)
        shared_ref[n * few : (n + 1) * few, :] = dot(rows[each:], sw_ref[...])


def down(hidden, weights, shared_down, side, slots):
    columns = weights.shape[2]
    whole = pl.BlockSpec(memory_space=pltpu.VMEM)
    return pl.pallas_call(
        functools.partial(down_kernel, side=side),
        in_specs=[whole] * 3,
        out_specs=(whole, whole),
        out_shape=(
            jax.ShapeDtypeStruct((slots, columns), BF16),
            jax.ShapeDtypeStruct((hidden.shape[1] * side - slots, columns), F32),
        ),
        name="down",
    )(hidden, weights, shared_down)


def combine_kernel(mix_ref, back_ref, shared_ref, out_ref):
    back = back_ref[...]
    routed = dot(mix_ref[0], back, TN) + dot(mix_ref[1], back, TN)
    out_ref[...] = (routed + shared_ref[...]).astype(BF16)


def combine(mix, back, shared):
    return pl.pallas_call(
        combine_kernel,
        out_shape=jax.ShapeDtypeStruct((mix.shape[2], back.shape[1]), BF16),
        name="combine",
    )(mix, back, shared)


def local(
    query_rows,
    key_rows,
    value_rows,
    cum_gate,
    out_weight,
    moe_input,
    moe_gain,
    routes,
    route_weight,
    expert_gate,
    expert_up,
    expert_down,
    shared_gate,
    shared_up,
    shared_down,
):
    groups = lax.axis_size("ep")
    peers = lax.axis_size("tp")
    side = math.isqrt(peers)
    along_x = [[y * side + x for x in range(side)] for y in range(side)]
    along_y = [[y * side + x for y in range(side)] for x in range(side)]
    ep_index = lax.axis_index("ep").astype(jnp.int32).reshape(1)
    tp_index = lax.axis_index("tp").astype(jnp.int32)
    side_index = jnp.stack([tp_index // side, tp_index % side])
    local_experts, _, hidden_each = expert_gate.shape
    columns = expert_down.shape[2]
    room = -(-CAP * local_experts // 8) * 8
    slot_count = groups * room
    key_value = jnp.concatenate([key_rows.T, value_rows.T], axis=0)
    kv_all = lax.all_gather(key_value, "ep", axis=0)
    slots, mix, tokens = route(
        side_index, moe_input, moe_gain.reshape(1, -1), routes.T, route_weight.T,
        side, groups, local_experts, room, columns,
    )
    arrived = exchanged(slots.reshape(groups, room, columns), "ep")
    pieces = spread_weights(
        side_index, expert_gate.transpose(0, 2, 1), expert_up.transpose(0, 2, 1), shared_gate.T, shared_up.T, side
    )
    pieces = [pieces[0]] + [
        lax.ppermute(
            pieces[k], "tp", [(row[x], row[(x + k) % side]) for row in along_x for x in range(side)]
        )
        for k in range(1, side)
    ]
    gathered = sent_to_all(arrived.reshape(slot_count, columns), "tp", along_y)
    parts = partial_products(side_index, gathered, tokens, pieces, local_experts, hidden_each)
    parts = exchanged(parts, "tp", along_x)
    own_hidden = activate(parts)
    hidden = sent_to_all(own_hidden, "tp")
    state = attention(ep_index, query_rows.T, kv_all, cum_gate, None, own_hidden)
    result, shared = down(hidden, expert_down, shared_down, side, slot_count)
    back = exchanged(result.reshape(groups, room, columns), "ep")
    heads = attention(ep_index, query_rows.T, kv_all, cum_gate, state, result)
    heads = sent_to_all(heads, "tp")
    mixer_out = projection(heads, out_weight)
    moe_out = combine(mix, back.reshape(slot_count, columns), shared)
    return (mixer_out, moe_out)


def solution(mesh):
    placed = (
        P("ep", "tp"),
        P("ep", "tp"),
        P("ep", "tp"),
        P("tp", None),
        P(None, "tp"),
        P("ep", None),
        P(),
        P("ep", None),
        P("ep", None),
        P("ep", None, "tp"),
        P("ep", None, "tp"),
        P("ep", None, "tp"),
        P(None, "tp"),
        P(None, "tp"),
        P(None, "tp"),
    )
    return jax.shard_map(
        local, mesh=mesh, in_specs=placed, out_specs=(P("ep", "tp"), P("ep", "tp")), check_vma=False
    )
```

```python
import functools
import math

import jax
import jax.numpy as jnp
from jax import lax
from jax.experimental import pallas as pl
from jax.experimental.pallas import tpu as pltpu
from jax.sharding import PartitionSpec as P

HEAD = 64
CAP = 9
LOG2E = 1.4426950408889634
neg_fill = -1e30
norm_eps = 1e-06
F32 = jnp.float32
BF16 = jnp.bfloat16
NT = (((1,), (1,)), ((), ()))
TN = (((0,), (0,)), ((), ()))
NN = (((1,), (0,)), ((), ()))


def dot(a, b, dims=NN):
    return lax.dot_general(a, b, dims, preferred_element_type=F32)


def exchanged(array, axis, among=None):
    return lax.all_to_all(array, axis, split_axis=0, concat_axis=0, tiled=True, axis_index_groups=among)


def sent_to_all(array, axis, among=None):
    count = len(among[0]) if among else lax.axis_size(axis)
    return exchanged(jnp.broadcast_to(array, (count, *array.shape)), axis, among)


def cost(flops, nbytes):
    return pl.CostEstimate(flops=flops, transcendentals=0, bytes_accessed=nbytes)


HEADROOM = 64.0
EXTRA = 16
GROUP = 2


def three(x):
    first = x.astype(BF16)
    rest = x - first.astype(F32)
    second = rest.astype(BF16)
    return first, second, (rest - second.astype(F32)).astype(BF16)


def attention_kernel(ep_ref, *refs, tile, opening):
    if opening:
        q_ref, kv_ref, gk_ref, g0_ref, _, acc_out, m_out, q_scr, m_scr, acc_scr = refs
    else:
        q_ref, kv_ref, gk_ref, g0_ref, acc_in, m_in, _, out_ref, q_scr, m_scr, acc_scr = refs
    step = pl.program_id(0)
    own = ep_ref[0]
    before = own // GROUP
    count = before // 2 if opening else before - before // 2
    rows = q_scr.shape[0]
    keys = kv_ref.shape[2] * GROUP

    def operands():
        kt = jnp.concatenate([kv_ref[n, :HEAD, :] for n in range(GROUP)], axis=1)
        row_id = lax.broadcasted_iota(jnp.int32, (2 * HEAD, keys), 0)
        both = jnp.concatenate([kv_ref[n] for n in range(GROUP)], axis=1)
        vt = jnp.where(row_id < HEAD, jnp.ones((), BF16), both)
        gate = (gk_ref[...] - g0_ref[:, :1]) * LOG2E
        row_id = lax.broadcasted_iota(jnp.int32, (EXTRA, keys), 0)
        gates = jnp.zeros((EXTRA, keys), F32)
        for n, piece in enumerate(three(gate)):
            gates = jnp.where(row_id == n, piece.astype(F32), gates)
        return jnp.concatenate([kt, kt, kt, gates.astype(BF16)], axis=0), vt

    def exact(source, target, diagonal):
        kx, vt = operands()
        for i in range(rows // tile):
            span = pl.ds(i * tile, tile)
            s = dot(q_scr[span, :], kx)
            if diagonal:
                q_pos = own * rows + i * tile + lax.broadcasted_iota(jnp.int32, (tile, keys), 0)
                k_pos = before * keys + lax.broadcasted_iota(jnp.int32, (tile, keys), 1)
                s = jnp.where(k_pos <= q_pos, s, neg_fill)
            top = jnp.max(s, axis=1, keepdims=True)
            if diagonal:
                p = jnp.exp2(s - top).astype(BF16)
                acc_scr[target, span, :] = dot(p, vt, NT)
                m_scr[span, :] = jnp.broadcast_to(top, (tile, m_scr.shape[1]))
            else:
                old = m_scr[span, :]
                new = jnp.maximum(old, top)
                p = jnp.exp2(s - new[:, :1]).astype(BF16)
                acc_scr[target, span, :] = acc_scr[source, span, :] * jnp.exp2(old - new) + dot(p, vt, NT)
                m_scr[span, :] = new

    @pl.when(step == 0)
    def _():
        for n, piece in enumerate(three(q_ref[...].T.astype(F32) * (LOG2E * HEAD**-0.5))):
            q_scr[:, n * HEAD : (n + 1) * HEAD] = piece
        q_scr[:, 3 * HEAD :] = jnp.full((rows, EXTRA), -1.0, BF16)
        if opening:
            exact(0, 0, True)
        else:
            acc_scr[0] = acc_in[...]
            m_scr[...] = m_in[...]

    @pl.when((step > 0) & (step <= count))
    def _():
        source = (step - 1) % 2
        target = step % 2
        kx, vt = operands()
        worst = jnp.full((8, 128), neg_fill, F32)
        for i in range(rows // tile):
            span = pl.ds(i * tile, tile)
            x = dot(q_scr[span, :], kx) - m_scr[span, :1]
            most = x[:, :128]
            for c in range(128, keys, 128):
                most = jnp.maximum(most, x[:, c : c + 128])
            worst = jnp.maximum(worst, jnp.max(most.reshape(tile // 8, 8, 128), axis=0))
            acc_scr[target, span, :] = acc_scr[source, span, :] + dot(jnp.exp2(x).astype(BF16), vt, NT)

        @pl.when(jnp.max(worst) > HEADROOM)
        def _():
            exact(source, target, False)

    @pl.when(step == pl.num_programs(0) - 1)
    def _():
        last = count % 2
        if opening:
            acc_out[...] = acc_scr[last]
            m_out[...] = m_scr[...]
        else:
            half = rows // 2
            top = acc_scr[last, :half, :]
            low = acc_scr[last, half:, :]
            out = jnp.concatenate(
                [top[:, HEAD:] / top[:, :HEAD], low[:, HEAD:] / low[:, :HEAD]], axis=1
            ).astype(BF16)
            for n in range(out_ref.shape[0]):
                out_ref[n] = out


def attention(ep_index, q_t, kv_all, cum_gate, state, after, copies):
    blocks, wide, keys = kv_all.shape
    rows = q_t.shape[1]
    opening = state is None
    steps = blocks // GROUP // 2

    def place(j, ep):
        before = ep[0] // GROUP
        half = before // 2
        if opening:
            return jnp.where(j == 0, before, jnp.maximum(jnp.minimum(j, half) - 1, 0))
        return jnp.minimum(half + jnp.maximum(j - 1, 0), jnp.maximum(before - 1, 0))

    flat = pl.BlockSpec((rows, 128), lambda j, ep: (0, 0))
    wide_f32 = jax.ShapeDtypeStruct((rows, 128), F32)
    sent = (copies, rows // 2, 2 * HEAD)
    return pl.pallas_call(
        functools.partial(attention_kernel, tile=384, opening=opening),
        grid_spec=pltpu.PrefetchScalarGridSpec(
            num_scalar_prefetch=1,
            grid=(steps + (0 if opening else 1),),
            in_specs=[
                pl.BlockSpec((HEAD, rows), lambda j, ep: (0, 0)),
                pl.BlockSpec((GROUP, wide, keys), lambda j, ep: (place(j, ep), 0, 0)),
                pl.BlockSpec((1, GROUP * keys), lambda j, ep: (0, place(j, ep))),
                pl.BlockSpec((1, keys), lambda j, ep: (0, ep[0])),
            ]
            + ([] if opening else [flat, flat])
            + [pl.BlockSpec(memory_space=pl.ANY)],
            out_specs=(flat, flat) if opening else pl.BlockSpec(sent, lambda j, ep: (0, 0, 0)),
            scratch_shapes=[
                pltpu.VMEM((rows, 3 * HEAD + EXTRA), BF16),
                pltpu.VMEM((rows, 128), F32),
                pltpu.VMEM((2, rows, 128), F32),
            ],
        ),
        out_shape=(wide_f32, wide_f32) if opening else jax.ShapeDtypeStruct(sent, BF16),
        compiler_params=pltpu.CompilerParams(dimension_semantics=("arbitrary",)),
        cost_estimate=cost(2 * rows * keys * blocks * 256, 4 << 20),
        name="attention_first" if opening else "attention_rest",
    )(ep_index, q_t, kv_all, cum_gate, cum_gate, *(state or ()), after)


def projection_kernel(heads_ref, w_ref, out_ref):
    count, half, _ = heads_ref.shape
    acc = jnp.zeros((half, 2 * w_ref.shape[1]), F32)
    blank = jnp.zeros((HEAD, w_ref.shape[1]), BF16)
    for h in range(count):
        w = w_ref[h * HEAD : (h + 1) * HEAD, :]
        both = jnp.concatenate(
            [jnp.concatenate([w, blank], axis=1), jnp.concatenate([blank, w], axis=1)], axis=0
        )
        acc = acc + dot(heads_ref[h], both)
    out_ref[:half, :] = acc[:, : w_ref.shape[1]].astype(BF16)
    out_ref[half:, :] = acc[:, w_ref.shape[1] :].astype(BF16)


def projection(heads, out_weight):
    count, half, _ = heads.shape
    columns = out_weight.shape[1]
    return pl.pallas_call(
        projection_kernel,
        out_shape=jax.ShapeDtypeStruct((2 * half, columns), BF16),
        cost_estimate=cost(2 * half * count * 128 * 256, 4 << 20),
        name="projection",
    )(heads, out_weight)


def spread_kernel(tp_ref, gate_ref, up_ref, *out_refs):
    side = len(out_refs)
    experts, hidden, width = gate_ref.shape
    part = width // side
    block = experts * hidden
    for k, out_ref in enumerate(out_refs):
        lanes = pl.ds(pl.multiple_of(lax.rem(lax.rem(tp_ref[0], side) + k, side) * part, part), part)
        out_ref[:block, :] = gate_ref[:, :, lanes].reshape(block, part)
        out_ref[block:, :] = up_ref[:, :, lanes].reshape(block, part)


def spread_weights(tp_index, gate_t, up_t, side):
    experts, hidden, width = gate_t.shape
    whole = pl.BlockSpec(memory_space=pltpu.VMEM)
    rows = 2 * experts * hidden
    return pl.pallas_call(
        spread_kernel,
        in_specs=[pl.BlockSpec(memory_space=pltpu.SMEM)] + [whole] * 2,
        out_specs=[whole] * side,
        out_shape=[jax.ShapeDtypeStruct((rows, width // side), BF16)] * side,
        name="spread",
    )(tp_index, gate_t, up_t)


def route_kernel(
    tp_ref, x_ref, gain_ref, routes_ref, weight_ref, sg_ref, su_ref, slot_ref, mix_ref, shared_ref, norm_scr,
    *, side, groups, local_experts, room,
):
    tokens = x_ref.shape[0]
    x = x_ref[...].astype(F32)
    scale = lax.rsqrt(jnp.mean(x * x, axis=1, keepdims=True) + norm_eps)
    normed = (x * scale * gain_ref[...]).astype(BF16)
    norm_scr[...] = normed
    columns = slot_ref.shape[1]
    start = pl.multiple_of((lax.rem(tp_ref[0], side) * side + lax.div(tp_ref[0], side)) * columns, columns)
    piece = norm_scr[:, pl.ds(start, columns)]
    slots = groups * room
    shape = (groups, room, tokens)
    within = lax.broadcasted_iota(jnp.int32, shape, 1)
    expert = lax.broadcasted_iota(jnp.int32, shape, 0) * local_experts + within % local_experts
    expert = expert.reshape(slots, tokens)
    turn = (within // local_experts).reshape(slots, tokens).astype(F32)
    hit = jnp.zeros((slots, tokens), F32)
    weight = jnp.zeros((slots, tokens), F32)
    for j in range(routes_ref.shape[0]):
        same = expert == routes_ref[j : j + 1, :]
        hit = hit + jnp.where(same, 1.0, 0.0)
        weight = weight + jnp.where(same, weight_ref[j : j + 1, :], 0.0)
    before = lax.broadcasted_iota(jnp.int32, (tokens, tokens), 0)
    after = lax.broadcasted_iota(jnp.int32, (tokens, tokens), 1)
    earlier = jnp.where(before < after, 1.0, 0.0).astype(BF16)
    rank = dot(hit.astype(BF16), earlier)
    chosen = jnp.where(rank == turn, hit, 0.0)
    slot_ref[...] = dot(chosen.astype(BF16), piece).astype(BF16)
    mix = chosen * weight
    coarse = mix.astype(BF16)
    mix_ref[0] = coarse
    mix_ref[1] = (mix - coarse.astype(F32)).astype(BF16)
    gate_val = dot(normed, sg_ref[...], NT)
    hidden = (gate_val / (1.0 + jnp.exp(-gate_val)) * dot(normed, su_ref[...], NT)).astype(BF16)
    few = shared_ref.shape[0]
    shared_ref[...] = jnp.concatenate([hidden[n * few : (n + 1) * few] for n in range(tokens // few)], axis=1)


def route(tp_index, x, gain, routes_t, weight_t, sg_t, su_t, side, groups, local_experts, room, columns):
    tokens, width = x.shape
    slots = groups * room
    whole = pl.BlockSpec(memory_space=pltpu.VMEM)
    return pl.pallas_call(
        functools.partial(route_kernel, side=side, groups=groups, local_experts=local_experts, room=room),
        in_specs=[pl.BlockSpec(memory_space=pltpu.SMEM)] + [whole] * 6,
        out_specs=(whole, whole, whole),
        out_shape=(
            jax.ShapeDtypeStruct((slots, columns), BF16),
            jax.ShapeDtypeStruct((2, slots, tokens), BF16),
            jax.ShapeDtypeStruct((tokens * sg_t.shape[0] // columns, columns), BF16),
        ),
        scratch_shapes=[pltpu.VMEM((tokens, width), BF16)],
        name="route",
    )(tp_index, x, gain, routes_t, weight_t, sg_t, su_t)


def by_expert(rows, count):
    own = lax.broadcasted_iota(jnp.int32, rows.shape, 0) % count
    return jnp.concatenate([jnp.where(own == e, rows, jnp.zeros((), rows.dtype)) for e in range(count)], axis=1)


def partial_kernel(tp_ref, rows_ref, *refs, count, hidden):
    side = len(refs) - 2
    out_ref, w_scr = refs[side:]
    wide = side * hidden
    depth = rows_ref.shape[2]
    for k in range(side):
        place = pl.multiple_of(lax.rem(lax.rem(tp_ref[0], side) + side - k, side) * hidden, hidden)
        for g in range(2):
            span = pl.ds(g * wide + place, hidden)
            for e in range(count):
                first = (g * count + e) * hidden
                for c in range(side):
                    lanes = (c * count + e) * depth
                    w_scr[span, lanes : lanes + depth] = refs[k][first : first + hidden, c * depth : (c + 1) * depth]
    each = out_ref.shape[1]
    for n in range(side):
        total = jnp.zeros((each, 2 * wide), F32)
        for c in range(side):
            spread = by_expert(rows_ref[c, n * each : (n + 1) * each, :], count)
            total = total + dot(spread, w_scr[:, c * count * depth : (c + 1) * count * depth], NT)
        out_ref[n] = total.astype(BF16)


def partial_products(tp_index, rows, weights, count, hidden):
    side = len(weights)
    whole = pl.BlockSpec(memory_space=pltpu.VMEM)
    return pl.pallas_call(
        functools.partial(partial_kernel, count=count, hidden=hidden),
        in_specs=[pl.BlockSpec(memory_space=pltpu.SMEM)] + [whole] * (1 + side),
        out_specs=whole,
        out_shape=jax.ShapeDtypeStruct((side, rows.shape[1] // side, 2 * side * hidden), BF16),
        scratch_shapes=[pltpu.VMEM((2 * side * hidden, count * side * rows.shape[2]), BF16)],
        name="partial",
    )(tp_index, rows, *weights)


def activate_kernel(parts_ref, shared_ref, out_ref):
    total = parts_ref[0].astype(F32)
    for t in range(1, parts_ref.shape[0]):
        total = total + parts_ref[t].astype(F32)
    rows, half = total.shape[0], out_ref.shape[2]
    gate_val = total[:, :half]
    hidden = (gate_val / (1.0 + jnp.exp(-gate_val)) * total[:, half:]).astype(BF16)
    for n in range(out_ref.shape[0]):
        out_ref[n, :rows, :] = hidden
        out_ref[n, rows:, :] = shared_ref[...]


def activate(parts, shared, copies):
    _, rows, width = parts.shape
    return pl.pallas_call(
        activate_kernel,
        out_shape=jax.ShapeDtypeStruct((copies, rows + shared.shape[0], width // 2), BF16),
        name="activate",
    )(parts, shared)


def down_kernel(hidden_ref, w_ref, sw_ref, out_ref, shared_ref, *, side):
    count, hidden, columns = w_ref.shape
    peers = hidden_ref.shape[0]
    each = out_ref.shape[0] // side
    w = w_ref[...].reshape(count * hidden, columns)
    for n in range(side):
        rows = jnp.concatenate([hidden_ref[y * side + n, :each, :] for y in range(side)], axis=1)
        out_ref[n * each : (n + 1) * each, :] = dot(by_expert(rows, count), w).astype(BF16)
    few = hidden_ref.shape[1] - each
    units = sw_ref.shape[0] // peers
    for n in range(shared_ref.shape[0] // few):
        rows = jnp.concatenate([hidden_ref[t, each:, n * units : (n + 1) * units] for t in range(peers)], axis=1)
        shared_ref[n * few : (n + 1) * few, :] = dot(rows, sw_ref[...])


def down(hidden, weights, shared_down, side, slots, tokens):
    columns = weights.shape[2]
    whole = pl.BlockSpec(memory_space=pltpu.VMEM)
    return pl.pallas_call(
        functools.partial(down_kernel, side=side),
        in_specs=[whole] * 3,
        out_specs=(whole, whole),
        out_shape=(
            jax.ShapeDtypeStruct((slots, columns), BF16),
            jax.ShapeDtypeStruct((tokens, columns), F32),
        ),
        name="down",
    )(hidden, weights, shared_down)


def combine_kernel(mix_ref, back_ref, shared_ref, out_ref):
    back = back_ref[...]
    routed = dot(mix_ref[0], back, TN) + dot(mix_ref[1], back, TN)
    out_ref[...] = (routed + shared_ref[...]).astype(BF16)


def combine(mix, back, shared):
    return pl.pallas_call(
        combine_kernel,
        out_shape=jax.ShapeDtypeStruct((mix.shape[2], back.shape[1]), BF16),
        name="combine",
    )(mix, back, shared)


def local(
    query_rows,
    key_rows,
    value_rows,
    cum_gate,
    out_weight,
    moe_input,
    moe_gain,
    routes,
    route_weight,
    expert_gate,
    expert_up,
    expert_down,
    shared_gate,
    shared_up,
    shared_down,
):
    groups = lax.axis_size("ep")
    peers = lax.axis_size("tp")
    side = math.isqrt(peers)
    along_x = [[y * side + x for x in range(side)] for y in range(side)]
    along_y = [[y * side + x for y in range(side)] for x in range(side)]
    ep_index = lax.axis_index("ep").astype(jnp.int32).reshape(1)
    tp_index = lax.axis_index("tp").astype(jnp.int32).reshape(1)
    local_experts, _, hidden_each = expert_gate.shape
    columns = expert_down.shape[2]
    room = -(-CAP * local_experts // 8) * 8
    slot_count = groups * room
    key_value = jnp.concatenate([key_rows.T, value_rows.T], axis=0)
    kv_all = lax.all_gather(key_value, "ep", axis=0)
    slots, mix, shared = route(
        tp_index, moe_input, moe_gain.reshape(1, -1), routes.T, route_weight.T, shared_gate.T, shared_up.T,
        side, groups, local_experts, room, columns,
    )
    arrived = exchanged(slots.reshape(groups, room, columns), "ep")
    pieces = spread_weights(tp_index, expert_gate.transpose(0, 2, 1), expert_up.transpose(0, 2, 1), side)
    pieces = list(pieces)
    for k in sorted(range(1, side), key=lambda k: -min(k, side - k)):
        steps = [(row[x], row[(x + k) % side]) for row in along_x for x in range(side)]
        pieces[k] = lax.ppermute(pieces[k], "tp", steps)
    gathered = sent_to_all(arrived.reshape(slot_count, columns), "tp", along_y)
    parts = partial_products(tp_index, gathered, pieces, local_experts, hidden_each)
    parts = exchanged(parts, "tp", along_x)
    own_hidden = activate(parts, shared, peers)
    hidden = exchanged(own_hidden, "tp")
    state = attention(ep_index, query_rows.T, kv_all, cum_gate, None, own_hidden, peers)
    result, shared = down(hidden, expert_down, shared_down, side, slot_count, moe_input.shape[0])
    back = exchanged(result.reshape(groups, room, columns), "ep")
    heads = attention(ep_index, query_rows.T, kv_all, cum_gate, state, result, peers)
    heads = exchanged(heads, "tp")
    mixer_out = projection(heads, out_weight)
    moe_out = combine(mix, back.reshape(slot_count, columns), shared)
    return (mixer_out, moe_out)


def solution(mesh):
    placed = (
        P("ep", "tp"),
        P("ep", "tp"),
        P("ep", "tp"),
        P("tp", None),
        P(None, "tp"),
        P("ep", None),
        P(),
        P("ep", None),
        P("ep", None),
        P("ep", None, "tp"),
        P("ep", None, "tp"),
        P("ep", None, "tp"),
        P(None, "tp"),
        P(None, "tp"),
        P(None, "tp"),
    )
    return jax.shard_map(
        local, mesh=mesh, in_specs=placed, out_specs=(P("ep", "tp"), P("ep", "tp")), check_vma=False
    )
```

```python
import functools
import math

import jax
import jax.numpy as jnp
from jax import lax
from jax.experimental import pallas as pl
from jax.experimental.pallas import tpu as pltpu
from jax.sharding import PartitionSpec as P

HEAD = 64
CAP = 9
LOG2E = 1.4426950408889634
neg_fill = -1e30
norm_eps = 1e-06
F32 = jnp.float32
BF16 = jnp.bfloat16
NT = (((1,), (1,)), ((), ()))
TN = (((0,), (0,)), ((), ()))
NN = (((1,), (0,)), ((), ()))


def dot(a, b, dims=NN):
    return lax.dot_general(a, b, dims, preferred_element_type=F32)


def exchanged(array, axis, among=None):
    return lax.all_to_all(array, axis, split_axis=0, concat_axis=0, tiled=True, axis_index_groups=among)


def cost(flops, nbytes):
    return pl.CostEstimate(flops=flops, transcendentals=0, bytes_accessed=nbytes)


HEADROOM = 64.0
EXTRA = 16
GROUP = 2


def three(x):
    first = x.astype(BF16)
    rest = x - first.astype(F32)
    second = rest.astype(BF16)
    return first, second, (rest - second.astype(F32)).astype(BF16)


def attention_kernel(ep_ref, *refs, tile, opening):
    if opening:
        q_ref, kv_ref, gk_ref, g0_ref, _, acc_out, m_out, q_scr, m_scr, acc_scr = refs
    else:
        q_ref, kv_ref, gk_ref, g0_ref, acc_in, m_in, _, out_ref, q_scr, m_scr, acc_scr = refs
    step = pl.program_id(0)
    own = ep_ref[0]
    before = own // GROUP
    count = before // 2 if opening else before - before // 2
    rows = q_scr.shape[0]
    keys = kv_ref.shape[2] * GROUP

    def operands():
        kt = jnp.concatenate([kv_ref[n, :HEAD, :] for n in range(GROUP)], axis=1)
        row_id = lax.broadcasted_iota(jnp.int32, (2 * HEAD, keys), 0)
        both = jnp.concatenate([kv_ref[n] for n in range(GROUP)], axis=1)
        vt = jnp.where(row_id < HEAD, jnp.ones((), BF16), both)
        gate = (gk_ref[...] - g0_ref[:, :1]) * LOG2E
        row_id = lax.broadcasted_iota(jnp.int32, (EXTRA, keys), 0)
        gates = jnp.zeros((EXTRA, keys), F32)
        for n, piece in enumerate(three(gate)):
            gates = jnp.where(row_id == n, piece.astype(F32), gates)
        return jnp.concatenate([kt, kt, kt, gates.astype(BF16)], axis=0), vt

    def exact(source, target, diagonal):
        kx, vt = operands()
        for i in range(rows // tile):
            span = pl.ds(i * tile, tile)
            s = dot(q_scr[span, :], kx)
            if diagonal:
                q_pos = own * rows + i * tile + lax.broadcasted_iota(jnp.int32, (tile, keys), 0)
                k_pos = before * keys + lax.broadcasted_iota(jnp.int32, (tile, keys), 1)
                s = jnp.where(k_pos <= q_pos, s, neg_fill)
            top = jnp.max(s, axis=1, keepdims=True)
            if diagonal:
                p = jnp.exp2(s - top).astype(BF16)
                acc_scr[target, span, :] = dot(p, vt, NT)
                m_scr[span, :] = jnp.broadcast_to(top, (tile, m_scr.shape[1]))
            else:
                old = m_scr[span, :]
                new = jnp.maximum(old, top)
                p = jnp.exp2(s - new[:, :1]).astype(BF16)
                acc_scr[target, span, :] = acc_scr[source, span, :] * jnp.exp2(old - new) + dot(p, vt, NT)
                m_scr[span, :] = new

    @pl.when(step == 0)
    def _():
        for n, piece in enumerate(three(q_ref[...].T.astype(F32) * (LOG2E * HEAD**-0.5))):
            q_scr[:, n * HEAD : (n + 1) * HEAD] = piece
        q_scr[:, 3 * HEAD :] = jnp.full((rows, EXTRA), -1.0, BF16)
        if opening:
            exact(0, 0, True)
        else:
            acc_scr[0] = acc_in[...]
            m_scr[...] = m_in[...]

    @pl.when((step > 0) & (step <= count))
    def _():
        source = (step - 1) % 2
        target = step % 2
        kx, vt = operands()
        worst = jnp.full((8, 128), neg_fill, F32)
        for i in range(rows // tile):
            span = pl.ds(i * tile, tile)
            x = dot(q_scr[span, :], kx) - m_scr[span, :1]
            most = x[:, :128]
            for c in range(128, keys, 128):
                most = jnp.maximum(most, x[:, c : c + 128])
            worst = jnp.maximum(worst, jnp.max(most.reshape(tile // 8, 8, 128), axis=0))
            acc_scr[target, span, :] = acc_scr[source, span, :] + dot(jnp.exp2(x).astype(BF16), vt, NT)

        @pl.when(jnp.max(worst) > HEADROOM)
        def _():
            exact(source, target, False)

    @pl.when(step == pl.num_programs(0) - 1)
    def _():
        last = count % 2
        if opening:
            acc_out[...] = acc_scr[last]
            m_out[...] = m_scr[...]
        else:
            half = rows // 2
            top = acc_scr[last, :half, :]
            low = acc_scr[last, half:, :]
            out = jnp.concatenate(
                [top[:, HEAD:] / top[:, :HEAD], low[:, HEAD:] / low[:, :HEAD]], axis=1
            ).astype(BF16)
            for n in range(out_ref.shape[0]):
                out_ref[n] = out


def attention(ep_index, q_t, kv_all, cum_gate, state, after, copies):
    blocks, wide, keys = kv_all.shape
    rows = q_t.shape[1]
    opening = state is None
    steps = blocks // GROUP // 2

    def place(j, ep):
        before = ep[0] // GROUP
        half = before // 2
        if opening:
            return jnp.where(j == 0, before, jnp.maximum(jnp.minimum(j, half) - 1, 0))
        return jnp.minimum(half + jnp.maximum(j - 1, 0), jnp.maximum(before - 1, 0))

    flat = pl.BlockSpec((rows, 128), lambda j, ep: (0, 0))
    wide_f32 = jax.ShapeDtypeStruct((rows, 128), F32)
    sent = (copies, rows // 2, 2 * HEAD)
    return pl.pallas_call(
        functools.partial(attention_kernel, tile=384, opening=opening),
        grid_spec=pltpu.PrefetchScalarGridSpec(
            num_scalar_prefetch=1,
            grid=(steps + (0 if opening else 1),),
            in_specs=[
                pl.BlockSpec((HEAD, rows), lambda j, ep: (0, 0)),
                pl.BlockSpec((GROUP, wide, keys), lambda j, ep: (place(j, ep), 0, 0)),
                pl.BlockSpec((1, GROUP * keys), lambda j, ep: (0, place(j, ep))),
                pl.BlockSpec((1, keys), lambda j, ep: (0, ep[0])),
            ]
            + ([] if opening else [flat, flat])
            + [pl.BlockSpec(memory_space=pl.ANY)],
            out_specs=(flat, flat) if opening else pl.BlockSpec(sent, lambda j, ep: (0, 0, 0)),
            scratch_shapes=[
                pltpu.VMEM((rows, 3 * HEAD + EXTRA), BF16),
                pltpu.VMEM((rows, 128), F32),
                pltpu.VMEM((2, rows, 128), F32),
            ],
        ),
        out_shape=(wide_f32, wide_f32) if opening else jax.ShapeDtypeStruct(sent, BF16),
        compiler_params=pltpu.CompilerParams(dimension_semantics=("arbitrary",)),
        cost_estimate=cost(2 * rows * keys * blocks * 256, 4 << 20),
        name="attention_first" if opening else "attention_rest",
    )(ep_index, q_t, kv_all, cum_gate, cum_gate, *(state or ()), after)


def projection_kernel(heads_ref, w_ref, out_ref):
    count, half, _ = heads_ref.shape
    columns = w_ref.shape[1]
    blank = jnp.zeros((HEAD, columns), BF16)
    acc = jnp.zeros((half, 2 * columns), F32)
    for h in range(0, count, 2):
        both = []
        for n in range(h, h + 2):
            w = w_ref[n * HEAD : (n + 1) * HEAD, :]
            both += [jnp.concatenate([w, blank], axis=1), jnp.concatenate([blank, w], axis=1)]
        rows = jnp.concatenate([heads_ref[h], heads_ref[h + 1]], axis=1)
        acc = acc + dot(rows, jnp.concatenate(both, axis=0))
    out_ref[:half, :] = acc[:, :columns].astype(BF16)
    out_ref[half:, :] = acc[:, columns:].astype(BF16)


def projection(heads, out_weight):
    count, half, _ = heads.shape
    columns = out_weight.shape[1]
    return pl.pallas_call(
        projection_kernel,
        out_shape=jax.ShapeDtypeStruct((2 * half, columns), BF16),
        cost_estimate=cost(2 * half * count * 128 * 256, 4 << 20),
        name="projection",
    )(heads, out_weight)


def spread_kernel(tp_ref, gate_ref, up_ref, *out_refs):
    side = len(out_refs)
    experts, hidden, width = gate_ref.shape
    part = width // side
    block = experts * hidden
    for k, out_ref in enumerate(out_refs):
        lanes = pl.ds(pl.multiple_of(lax.rem(lax.rem(tp_ref[0], side) + k, side) * part, part), part)
        out_ref[:block, :] = gate_ref[:, :, lanes].reshape(block, part)
        out_ref[block:, :] = up_ref[:, :, lanes].reshape(block, part)


def spread_weights(tp_index, gate_t, up_t, side):
    experts, hidden, width = gate_t.shape
    whole = pl.BlockSpec(memory_space=pltpu.VMEM)
    rows = 2 * experts * hidden
    return pl.pallas_call(
        spread_kernel,
        in_specs=[pl.BlockSpec(memory_space=pltpu.SMEM)] + [whole] * 2,
        out_specs=[whole] * side,
        out_shape=[jax.ShapeDtypeStruct((rows, width // side), BF16)] * side,
        name="spread",
    )(tp_index, gate_t, up_t)


def normed_rows(x_ref, gain_ref):
    x = x_ref[...].astype(F32)
    scale = lax.rsqrt(jnp.mean(x * x, axis=1, keepdims=True) + norm_eps)
    return (x * scale * gain_ref[...]).astype(BF16)


def slot_choice(routes_ref, groups, local_experts, room):
    tokens = routes_ref.shape[1]
    shape = (groups, room, tokens)
    within = lax.broadcasted_iota(jnp.int32, shape, 1)
    expert = lax.broadcasted_iota(jnp.int32, shape, 0) * local_experts + within % local_experts
    expert = expert.reshape(groups * room, tokens)
    turn = (within // local_experts).reshape(groups * room, tokens).astype(F32)
    same = [expert == routes_ref[j : j + 1, :] for j in range(routes_ref.shape[0])]
    hit = sum(jnp.where(one, 1.0, 0.0) for one in same)
    before = lax.broadcasted_iota(jnp.int32, (tokens, tokens), 0)
    after = lax.broadcasted_iota(jnp.int32, (tokens, tokens), 1)
    rank = dot(hit.astype(BF16), jnp.where(before < after, 1.0, 0.0).astype(BF16))
    return jnp.where(rank == turn, hit, 0.0), same


def route_kernel(tp_ref, x_ref, gain_ref, routes_ref, slot_ref, norm_scr, *, side, groups, local_experts, room):
    norm_scr[...] = normed_rows(x_ref, gain_ref)
    columns = slot_ref.shape[1]
    start = pl.multiple_of((lax.rem(tp_ref[0], side) * side + lax.div(tp_ref[0], side)) * columns, columns)
    chosen, _ = slot_choice(routes_ref, groups, local_experts, room)
    slot_ref[...] = dot(chosen.astype(BF16), norm_scr[:, pl.ds(start, columns)]).astype(BF16)


def route(tp_index, x, gain, routes_t, side, groups, local_experts, room, columns):
    whole = pl.BlockSpec(memory_space=pltpu.VMEM)
    return pl.pallas_call(
        functools.partial(route_kernel, side=side, groups=groups, local_experts=local_experts, room=room),
        in_specs=[pl.BlockSpec(memory_space=pltpu.SMEM)] + [whole] * 3,
        out_specs=whole,
        out_shape=jax.ShapeDtypeStruct((groups * room, columns), BF16),
        scratch_shapes=[pltpu.VMEM(x.shape, BF16)],
        name="route",
    )(tp_index, x, gain, routes_t)


def mixture_kernel(
    x_ref, gain_ref, routes_ref, weight_ref, sg_ref, su_ref, mix_ref, shared_ref, *, groups, local_experts, room
):
    chosen, same = slot_choice(routes_ref, groups, local_experts, room)
    mix = chosen * sum(jnp.where(one, weight_ref[j : j + 1, :], 0.0) for j, one in enumerate(same))
    coarse = mix.astype(BF16)
    mix_ref[0] = coarse
    mix_ref[1] = (mix - coarse.astype(F32)).astype(BF16)
    normed = normed_rows(x_ref, gain_ref)
    gate_val = dot(normed, sg_ref[...], NT)
    hidden = (gate_val / (1.0 + jnp.exp(-gate_val)) * dot(normed, su_ref[...], NT)).astype(BF16)
    few = shared_ref.shape[0]
    pieces = [hidden[n * few : (n + 1) * few] for n in range(hidden.shape[0] // few)]
    shared_ref[...] = jnp.concatenate(pieces, axis=1)


def mixture(x, gain, routes_t, weight_t, sg_t, su_t, groups, local_experts, room, columns):
    tokens = x.shape[0]
    return pl.pallas_call(
        functools.partial(mixture_kernel, groups=groups, local_experts=local_experts, room=room),
        out_shape=(
            jax.ShapeDtypeStruct((2, groups * room, tokens), BF16),
            jax.ShapeDtypeStruct((tokens * sg_t.shape[0] // columns, columns), BF16),
        ),
        name="mixture",
    )(x, gain, routes_t, weight_t, sg_t, su_t)


def by_expert(rows, count):
    own = lax.broadcasted_iota(jnp.int32, rows.shape, 0) % count
    return jnp.concatenate([jnp.where(own == e, rows, jnp.zeros((), rows.dtype)) for e in range(count)], axis=1)


def compact_kernel(rows_ref, out_ref, scr):
    sources = rows_ref.shape[0]
    used = out_ref.shape[1] // sources
    for n in range(sources):
        scr[n * used : (n + 1) * used, :] = rows_ref[n].astype(F32)[:used]
    rows = scr[...].astype(BF16)
    for n in range(out_ref.shape[0]):
        out_ref[n] = rows


def compact(rows, used, copies):
    sources, _, columns = rows.shape
    return pl.pallas_call(
        compact_kernel,
        out_shape=jax.ShapeDtypeStruct((copies, sources * used, columns), BF16),
        scratch_shapes=[pltpu.VMEM((sources * used, columns), F32)],
        name="compact",
    )(rows)


def partial_kernel(tp_ref, rows_ref, *refs, count, hidden):
    side = len(refs) - 2
    out_ref, w_scr = refs[side:]
    wide = side * hidden
    depth = rows_ref.shape[2]
    for k in range(side):
        place = pl.multiple_of(lax.rem(lax.rem(tp_ref[0], side) + side - k, side) * hidden, hidden)
        for g in range(2):
            span = pl.ds(g * wide + place, hidden)
            for e in range(count):
                first = (g * count + e) * hidden
                for c in range(side):
                    lanes = (c * count + e) * depth
                    w_scr[span, lanes : lanes + depth] = refs[k][first : first + hidden, c * depth : (c + 1) * depth]
    each = out_ref.shape[1]
    for n in range(side):
        total = jnp.zeros((each, 2 * wide), F32)
        for c in range(side):
            spread = by_expert(rows_ref[c, n * each : (n + 1) * each, :], count)
            total = total + dot(spread, w_scr[:, c * count * depth : (c + 1) * count * depth], NT)
        out_ref[n] = total.astype(BF16)


def partial_products(tp_index, rows, weights, count, hidden):
    side = len(weights)
    whole = pl.BlockSpec(memory_space=pltpu.VMEM)
    return pl.pallas_call(
        functools.partial(partial_kernel, count=count, hidden=hidden),
        in_specs=[pl.BlockSpec(memory_space=pltpu.SMEM)] + [whole] * (1 + side),
        out_specs=whole,
        out_shape=jax.ShapeDtypeStruct((side, rows.shape[1] // side, 2 * side * hidden), BF16),
        scratch_shapes=[pltpu.VMEM((2 * side * hidden, count * side * rows.shape[2]), BF16)],
        name="partial",
    )(tp_index, rows, *weights)


def activate_kernel(parts_ref, shared_ref, out_ref):
    total = parts_ref[0].astype(F32)
    for t in range(1, parts_ref.shape[0]):
        total = total + parts_ref[t].astype(F32)
    rows, half = total.shape[0], out_ref.shape[2]
    gate_val = total[:, :half]
    hidden = (gate_val / (1.0 + jnp.exp(-gate_val)) * total[:, half:]).astype(BF16)
    for n in range(out_ref.shape[0]):
        out_ref[n, :rows, :] = hidden
        out_ref[n, rows:, :] = shared_ref[...]


def activate(parts, shared, copies):
    _, rows, width = parts.shape
    return pl.pallas_call(
        activate_kernel,
        out_shape=jax.ShapeDtypeStruct((copies, rows + shared.shape[0], width // 2), BF16),
        name="activate",
    )(parts, shared)


def down_kernel(hidden_ref, w_ref, sw_ref, out_ref, shared_ref, scr, *, side, used):
    count, hidden, columns = w_ref.shape
    peers = hidden_ref.shape[0]
    sources, room, _ = out_ref.shape
    few = hidden_ref.shape[1] - sources * used // side
    each = sources * used // side
    w = w_ref[...].reshape(count * hidden, columns)
    scr[each:, :] = jnp.zeros((scr.shape[0] - each, columns), F32)
    for n in range(side):
        rows = jnp.concatenate([hidden_ref[y * side + n, :each, :] for y in range(side)], axis=1)
        scr[:each, :] = dot(by_expert(rows, count), w)
        for m in range(sources // side):
            out_ref[n * (sources // side) + m] = scr[m * used : m * used + room, :].astype(BF16)
    units = sw_ref.shape[0] // peers
    for n in range(shared_ref.shape[0] // few):
        rows = jnp.concatenate([hidden_ref[t, each:, n * units : (n + 1) * units] for t in range(peers)], axis=1)
        shared_ref[n * few : (n + 1) * few, :] = dot(rows, sw_ref[...])


def down(hidden, weights, shared_down, side, groups, used, room, tokens):
    columns = weights.shape[2]
    whole = pl.BlockSpec(memory_space=pltpu.VMEM)
    return pl.pallas_call(
        functools.partial(down_kernel, side=side, used=used),
        in_specs=[whole] * 3,
        out_specs=(whole, whole),
        out_shape=(
            jax.ShapeDtypeStruct((groups, room, columns), BF16),
            jax.ShapeDtypeStruct((tokens, columns), F32),
        ),
        scratch_shapes=[pltpu.VMEM((groups // side * used + 8, columns), F32)],
        name="down",
    )(hidden, weights, shared_down)


def combine_kernel(mix_ref, back_ref, shared_ref, out_ref):
    back = back_ref[...]
    routed = dot(mix_ref[0], back, TN) + dot(mix_ref[1], back, TN)
    out_ref[...] = (routed + shared_ref[...]).astype(BF16)


def combine(mix, back, shared):
    return pl.pallas_call(
        combine_kernel,
        out_shape=jax.ShapeDtypeStruct((mix.shape[2], back.shape[1]), BF16),
        name="combine",
    )(mix, back, shared)


def local(
    query_rows,
    key_rows,
    value_rows,
    cum_gate,
    out_weight,
    moe_input,
    moe_gain,
    routes,
    route_weight,
    expert_gate,
    expert_up,
    expert_down,
    shared_gate,
    shared_up,
    shared_down,
):
    groups = lax.axis_size("ep")
    peers = lax.axis_size("tp")
    side = math.isqrt(peers)
    along_x = [[y * side + x for x in range(side)] for y in range(side)]
    along_y = [[y * side + x for y in range(side)] for x in range(side)]
    ep_index = lax.axis_index("ep").astype(jnp.int32).reshape(1)
    tp_index = lax.axis_index("tp").astype(jnp.int32).reshape(1)
    local_experts, _, hidden_each = expert_gate.shape
    columns = expert_down.shape[2]
    used = CAP * local_experts
    room = -(-used // 8) * 8
    slot_count = groups * room
    key_value = jnp.concatenate([key_rows.T, value_rows.T], axis=0)
    kv_all = lax.all_gather(key_value, "ep", axis=0)
    gain = moe_gain.reshape(1, -1)
    slots = route(tp_index, moe_input, gain, routes.T, side, groups, local_experts, room, columns)
    mix, shared = mixture(
        moe_input, gain, routes.T, route_weight.T, shared_gate.T, shared_up.T,
        groups, local_experts, room, columns,
    )
    arrived = exchanged(slots.reshape(groups, room, columns), "ep")
    pieces = spread_weights(tp_index, expert_gate.transpose(0, 2, 1), expert_up.transpose(0, 2, 1), side)
    pieces = list(pieces)
    for k in sorted(range(1, side), key=lambda k: -min(k, side - k)):
        steps = [(row[x], row[(x + k) % side]) for row in along_x for x in range(side)]
        pieces[k] = lax.ppermute(pieces[k], "tp", steps)
    gathered = exchanged(compact(arrived, used, side), "tp", along_y)
    parts = partial_products(tp_index, gathered, pieces, local_experts, hidden_each)
    parts = exchanged(parts, "tp", along_x)
    own_hidden = activate(parts, shared, peers)
    hidden = exchanged(own_hidden, "tp")
    state = attention(ep_index, query_rows.T, kv_all, cum_gate, None, own_hidden, peers)
    result, shared = down(
        hidden, expert_down, shared_down, side, groups, used, room, moe_input.shape[0]
    )
    back = exchanged(result, "ep")
    heads = attention(ep_index, query_rows.T, kv_all, cum_gate, state, result, peers)
    heads = exchanged(heads, "tp")
    mixer_out = projection(heads, out_weight)
    moe_out = combine(mix, back.reshape(slot_count, columns), shared)
    return (mixer_out, moe_out)


def solution(mesh):
    placed = (
        P("ep", "tp"),
        P("ep", "tp"),
        P("ep", "tp"),
        P("tp", None),
        P(None, "tp"),
        P("ep", None),
        P(),
        P("ep", None),
        P("ep", None),
        P("ep", None, "tp"),
        P("ep", None, "tp"),
        P("ep", None, "tp"),
        P(None, "tp"),
        P(None, "tp"),
        P(None, "tp"),
    )
    return jax.shard_map(
        local, mesh=mesh, in_specs=placed, out_specs=(P("ep", "tp"), P("ep", "tp")), check_vma=False
    )
```
